32 devices in a mesh: fs: 8 (over z, y), tp: 4 (over x, core).
Axes of the slice: x: 2, y: 2, z: 4, core: 2. Of those that a mesh axis runs over, the one named last changes fastest.
Arguments:
- block_input: bfloat16 [1536, 2048], P('fs'), may hold values from -6 to 6
- query_cotangent: bfloat16 [1536, 1024], P('fs', 'tp'), may hold values from -0.15625 to 0.15625
- key_cotangent: bfloat16 [1536, 1024], P('fs', 'tp'), may hold values from -0.15625 to 0.15625
- query_factor: bfloat16 [2048, 256], P('fs'), may hold values from -0.125 to 0.125
- key_factor: bfloat16 [2048, 256], P('fs'), may hold values from -0.125 to 0.125
- query_first: float32 [256, 1024], P('fs', 'tp'), may hold values from -0.6 to 0.6
- query_second: float32 [256, 1024], P('fs', 'tp'), may hold values from 0.005 to 0.03
- key_first: float32 [256, 1024], P('fs', 'tp'), may hold values from -0.6 to 0.6
- key_second: float32 [256, 1024], P('fs', 'tp'), may hold values from 0.005 to 0.03
- query_weight: float32 [2048, 1024], P('fs', 'tp'), may hold values from -0.125 to 0.125
- key_weight: float32 [2048, 1024], P('fs', 'tp'), may hold values from -0.125 to 0.125
Outputs:
- query_update: float32 [2048, 1024], P('fs', 'tp')
- query_new: float32 [2048, 1024], P('fs', 'tp')
- query_copy: bfloat16 [2048, 1024], P(None, 'tp')
- query_first_new: float32 [256, 1024], P('fs', 'tp')
- query_second_new: float32 [256, 1024], P('fs', 'tp')
- key_update: float32 [2048, 1024], P('fs', 'tp')
- key_new: float32 [2048, 1024], P('fs', 'tp')
- key_copy: bfloat16 [2048, 1024], P(None, 'tp')
- key_first_new: float32 [256, 1024], P('fs', 'tp')
- key_second_new: float32 [256, 1024], P('fs', 'tp')
The draws below stay inside these ranges and needn't reach their ends.
All inputs are finite; a program needn't handle non-finite values.
Results may differ from the reference program's by a relative error of at most 0.0005.
Values may be sent and summed in bfloat16 or wider, within the bound.
A program may use at most 64 MiB of HBM per device.

```python
import math
import jax
import jax.numpy as jnp
from jax import lax

D = 2048
WIDTH = 1024
RANK = 256
TOKENS = 1536


def block_levels(own_key, extent, split, smallest, high):
    def one(axis_at, shards_of):
        steps = jax.random.uniform(jax.random.fold_in(jax.random.fold_in(own_key, 6), axis_at), (shards_of,), jnp.float32, smallest / len(split), high / len(split))
        return jnp.repeat(jnp.exp(steps), extent[axis_at] // shards_of).reshape((-1,) + (1,) * (len(extent) - axis_at - 1))

    loudness = one(*split[0])
    for cut in split[1:]:
        loudness = loudness * one(*cut)
    return loudness


def gaussian(stream_key, shape, width, limit, pieces=(), kind=jnp.bfloat16):
    factor_of = block_levels(stream_key, shape, pieces, -0.22, 0.18) if pieces else 1.0
    array = jax.random.normal(stream_key, shape, jnp.float32) * width * factor_of
    return jnp.minimum(jnp.maximum(array, -limit), limit).astype(kind)


def setup_inputs(seed: int = 0) -> dict:
    keys = jax.random.split(jax.random.key(seed), 12)
    return {
        "block_input": gaussian(keys[0], (TOKENS, D), 1.0, 6.0, ((0, 8),)),
        "query_cotangent": gaussian(keys[1], (TOKENS, WIDTH), TOKENS ** -0.5, 0.15625, ((0, 8), (1, 4))),
        "key_cotangent": gaussian(keys[2], (TOKENS, WIDTH), TOKENS ** -0.5, 0.15625, ((0, 8), (1, 4))),
        "query_factor": gaussian(keys[3], (D, RANK), D ** -0.5, 0.125, ((0, 8),)),
        "key_factor": gaussian(keys[4], (D, RANK), D ** -0.5, 0.125, ((0, 8),)),
        "query_first": gaussian(keys[5], (RANK, WIDTH), 0.1, 0.6, ((0, 8), (1, 4)), jnp.float32),
        "query_second": jnp.clip(jnp.exp(math.log(0.03) - 1.7917595 * jax.random.uniform(keys[6], (RANK, WIDTH), jnp.float32) ** block_levels(keys[6], (RANK, WIDTH), ((0, 8), (1, 4)), -0.2, 0.2)), 0.005, 0.03),
        "key_first": gaussian(keys[7], (RANK, WIDTH), 0.1, 0.6, ((0, 8), (1, 4)), jnp.float32),
        "key_second": jnp.clip(jnp.exp(math.log(0.03) - 1.7917595 * jax.random.uniform(keys[8], (RANK, WIDTH), jnp.float32) ** block_levels(keys[8], (RANK, WIDTH), ((0, 8), (1, 4)), -0.2, 0.2)), 0.005, 0.03),
        "query_weight": gaussian(keys[9], (D, WIDTH), D ** -0.5, 0.125, ((0, 8), (1, 4)), jnp.float32),
        "key_weight": gaussian(keys[10], (D, WIDTH), D ** -0.5, 0.125, ((0, 8), (1, 4)), jnp.float32),
    }


beta_one = 0.9
beta_two = 0.99
denom_floor = 0.001
scale_floor = 0.5
learn_rate = 0.02

def one_update(block_input, cotangent, factor, first, second, weight):
    gradient = jnp.dot(block_input.T, cotangent, preferred_element_type=jnp.float32)
    factor_wide = factor.astype(jnp.float32)
    small = jnp.dot(factor_wide.T, gradient, precision=lax.Precision.HIGHEST)
    first_new = beta_one * first + (1.0 - beta_one) * small
    second_new = beta_two * second + (1.0 - beta_two) * small * small
    direction = first_new / (jnp.sqrt(second_new) + denom_floor)
    spread = jnp.sqrt(jnp.sum(direction * direction) / direction.size)
    scale = 1.0 / jnp.maximum(spread, scale_floor)
    update = -scale * jnp.dot(factor_wide, direction, precision=lax.Precision.HIGHEST)
    fresh = weight + learn_rate * update
    return (update, fresh, fresh.astype(jnp.bfloat16), first_new, second_new)

def reference(block_input, query_cotangent, key_cotangent, query_factor, key_factor, query_first, query_second, key_first, key_second, query_weight, key_weight):
    query_out = one_update(block_input, query_cotangent, query_factor, query_first, query_second, query_weight)
    key_out = one_update(block_input, key_cotangent, key_factor, key_first, key_second, key_weight)
    return (query_out[0], query_out[1], query_out[2], query_out[3], query_out[4], key_out[0], key_out[1], key_out[2], key_out[3], key_out[4])
```

```python
import functools

import jax
import jax.numpy as jnp
from jax import lax
from jax.experimental import pallas as pl
from jax.experimental.pallas import tpu as pltpu
from jax.sharding import PartitionSpec as P

beta_one = 0.9
beta_two = 0.99
denom_floor = 0.001
scale_floor = 0.5
learn_rate = 0.02
MESH = pl.DeviceIdType.MESH
ANY = pl.BlockSpec(memory_space=pl.ANY)


def moments(small, first, second):
    first_new = beta_one * first + (1.0 - beta_one) * small
    second_new = beta_two * second + (1.0 - beta_two) * small * small
    direction = first_new / (jnp.sqrt(second_new) + denom_floor)
    return (first_new, second_new, direction)


def split_two(values):
    upper = values.astype(jnp.bfloat16)
    lower = (values - upper.astype(jnp.float32)).astype(jnp.bfloat16)
    return (upper, lower)


def ring_place(index, n):
    odd = index % 2
    along = index // 2
    return (1 - odd) * along + odd * (n - 1 - along)


def ring_index(place, n):
    back = place // (n // 2)
    return (1 - back) * (2 * place) + back * (2 * (n - 1 - place) + 1)


class Ring:
    def __init__(self, n, me, own, slot, send, recv):
        self.n, self.own, self.slot, self.send, self.recv = n, own, slot, send, recv
        self.me = me
        self.place = ring_place(me, n)
        self.last = n // 2

    def active(self, step, way, half):
        return step < self.last or (step == self.last and way == half)

    def owner(self, step, way):
        shift = -step if way == 0 else step
        return ring_index((self.place + shift + self.n) % self.n, self.n)

    def copy(self, step, way, half):
        shift = 1 if way == 0 else self.n - 1
        to = ring_index((self.place + shift) % self.n, self.n)
        if step == 1:
            owner, src = self.me, self.own(half)
        else:
            owner = self.owner(step - 1, way)
            src = self.slot(owner, half)
        return pltpu.make_async_remote_copy(
            src_ref=src,
            dst_ref=self.slot(owner, half),
            send_sem=self.send.at[way, step - 1, half],
            recv_sem=self.recv.at[way, step - 1, half],
            device_id={"fs": to},
            device_id_type=MESH,
        )

    def begin(self, half):
        for way in range(2):
            if self.active(1, way, half):
                self.copy(1, way, half).start()

    def step(self, step, arrived):
        for half in range(2):
            for way in range(2):
                if self.active(step, way, half):
                    self.copy(step, way, half).wait_recv()
                    if self.active(step + 1, way, half):
                        self.copy(step + 1, way, half).start()
                    arrived(self.owner(step, way), half)

    def finish(self):
        for step in range(1, self.last + 1):
            for way in range(2):
                for half in range(2):
                    if self.active(step, way, half):
                        self.copy(step, way, half).wait_send()


def fused(
    n,
    tps,
    x_in,
    cq_in,
    ck_in,
    fq_in,
    fk_in,
    q1_in,
    q2_in,
    k1_in,
    k2_in,
    wq_in,
    wk_in,
    uq_out,
    nq_out,
    cq_out,
    q1_out,
    q2_out,
    uk_out,
    nk_out,
    ck_out,
    k1_out,
    k2_out,
    x,
    cot,
    fac,
    first,
    second,
    weight,
    gathered,
    mix,
    part,
    landed,
    dirs,
    squares,
    update,
    fresh,
    copies,
    in_sem,
    out_sem,
    copy_sem,
    ring_a_send,
    ring_a_recv,
    ring_e_send,
    ring_e_recv,
    mix_send,
    mix_recv,
    part_send,
    part_recv,
    dir_send,
    dir_recv,
    sq_send,
    sq_recv,
):
    me = lax.axis_index("fs")
    tp = lax.axis_index("tp")
    core = tp % 2
    rows = fac.shape[1]
    half_rows = rows // 2
    rank_rows = first.shape[1]
    rank = n * rank_rows
    width = cot.shape[2]

    loads = [
        pltpu.make_async_copy(src, dst, in_sem.at[i])
        for i, (src, dst) in enumerate(
            (
                (fq_in, fac.at[0]),
                (fk_in, fac.at[1]),
                (x_in, x),
                (cq_in, cot.at[0]),
                (ck_in, cot.at[1]),
                (q1_in, first.at[0]),
                (k1_in, first.at[1]),
                (q2_in, second.at[0]),
                (k2_in, second.at[1]),
                (wq_in, weight.at[0]),
                (wk_in, weight.at[1]),
            )
        )
    ]
    for load in loads:
        load.start()

    barrier = pltpu.get_barrier_semaphore()
    for k in range(1, n):
        pl.semaphore_signal(barrier, inc=1, device_id={"fs": (me + k) % n}, device_id_type=MESH)
    for k in range(1, tps):
        pl.semaphore_signal(barrier, inc=1, device_id={"tp": (tp + k) % tps}, device_id_type=MESH)
    pl.semaphore_wait(barrier, n + tps - 2)

    loads[0].wait()
    loads[1].wait()
    ring = Ring(
        n,
        me,
        lambda half: fac.at[core, pl.ds(half * half_rows, half_rows)],
        lambda owner, half: gathered.at[owner, pl.ds(half * half_rows, half_rows)],
        ring_a_send,
        ring_a_recv,
    )
    ring.begin(0)
    ring.begin(1)
    loads[2].wait()

    def product(owner, low, size, block):
        columns = pl.ds(pl.multiple_of(owner * rows + low, 128), size)
        mix[core] += jnp.dot(x[:, columns], block, preferred_element_type=jnp.float32)

    mix[core] = jnp.dot(
        x[:, pl.ds(pl.multiple_of(me * rows, 128), rows)],
        fac[core],
        preferred_element_type=jnp.float32,
    )
    for step in range(1, n // 2 + 1):
        seen = []
        ring.step(step, lambda owner, half: seen.append((owner, half)))
        if step < n // 2:
            for way in range(2):
                owner = ring.owner(step, way)
                product(owner, 0, rows, gathered[owner])
        else:
            product(ring.owner(step, 0), 0, rows, gathered[ring.owner(step, 0)])

    swap = pltpu.make_async_remote_copy(
        src_ref=mix.at[core],
        dst_ref=mix.at[core],
        send_sem=mix_send,
        recv_sem=mix_recv,
        device_id={"tp": tp + 1 - 2 * core},
        device_id_type=MESH,
    )
    swap.start()
    ring.finish()
    for load in loads[3:]:
        load.wait()
    swap.wait()

    contract = (((0,), (0,)), ((), ()))
    for p in range(2):
        upper, lower = split_two(mix[p])
        total = lax.dot_general(upper, cot[p], contract, preferred_element_type=jnp.float32)
        total += lax.dot_general(lower, cot[p], contract, preferred_element_type=jnp.float32)
        part[:, p] = total.reshape(n, rank_rows, width)

    def share(k):
        to = (me + k) % n
        return pltpu.make_async_remote_copy(
            src_ref=part.at[to],
            dst_ref=landed.at[me],
            send_sem=part_send.at[k - 1],
            recv_sem=part_recv.at[k - 1],
            device_id={"fs": to},
            device_id_type=MESH,
        )

    for k in range(1, n):
        share(k).start()
    small = part[me]
    for k in range(1, n):
        share(k).wait_recv()
        small += landed[(me - k + n) % n]

    first_new, second_new, direction = moments(small, first[...], second[...])
    dirs[me] = direction

    def spread(k):
        return pltpu.make_async_remote_copy(
            src_ref=dirs.at[me],
            dst_ref=dirs.at[me],
            send_sem=dir_send.at[k - 1],
            recv_sem=dir_recv.at[k - 1],
            device_id={"fs": (me + k) % n},
            device_id_type=MESH,
        )

    for k in range(1, n):
        spread(k).start()
    first[...] = first_new
    second[...] = second_new
    outs = [
        pltpu.make_async_copy(src, dst, out_sem.at[i])
        for i, (src, dst) in enumerate(
            (
                (first.at[0], q1_out),
                (first.at[1], k1_out),
                (second.at[0], q2_out),
                (second.at[1], k2_out),
                (update.at[0], uq_out),
                (update.at[1], uk_out),
                (fresh.at[0], nq_out),
                (fresh.at[1], nk_out),
            )
        )
    ]
    for out in outs[:4]:
        out.start()
    for k in range(1, n):
        share(k).wait_send()
    for k in range(1, n):
        spread(k).wait_recv()

    full = [dirs[:, p].reshape(rank, width) for p in range(2)]
    for p in range(2):
        squares[tp, p] = jnp.sum((full[p] * full[p]).reshape(rank // 8, 8, width), axis=0)

    def tell(k):
        return pltpu.make_async_remote_copy(
            src_ref=squares.at[tp],
            dst_ref=squares.at[tp],
            send_sem=sq_send.at[k - 1],
            recv_sem=sq_recv.at[k - 1],
            device_id={"tp": (tp + k) % tps},
            device_id_type=MESH,
        )

    for k in range(1, tps):
        tell(k).start()
    for p in range(2):
        upper, lower = split_two(full[p])
        total = jnp.dot(fac[p], upper, preferred_element_type=jnp.float32)
        update[p] = total + jnp.dot(fac[p], lower, preferred_element_type=jnp.float32)
    for k in range(1, tps):
        tell(k).wait_recv()

    ring = Ring(
        n,
        me,
        lambda half: copies.at[me, half],
        lambda owner, half: copies.at[owner, half],
        ring_e_send,
        ring_e_recv,
    )
    targets = (cq_out, ck_out)

    def put(owner, half):
        return pltpu.make_async_copy(
            copies.at[owner, half],
            targets[half].at[pl.ds(pl.multiple_of(owner * rows, 16), rows)],
            copy_sem.at[owner, half],
        )

    for p in range(2):
        square = jnp.sum(jnp.sum(squares[:, p], axis=0), keepdims=True)
        scale = 1.0 / jnp.maximum(jnp.sqrt(square / (rank * width * tps)), scale_floor)
        step = -scale * update[p]
        made = weight[p] + learn_rate * step
        copies[me, p] = made.astype(jnp.bfloat16)
        ring.begin(p)
        update[p] = step
        fresh[p] = made
        put(me, p).start()
        outs[4 + p].start()
        outs[6 + p].start()

    for step in range(1, n // 2 + 1):
        ring.step(step, lambda owner, half: put(owner, half).start())
    for k in range(1, n):
        spread(k).wait_send()
    for k in range(1, tps):
        tell(k).wait_send()
    ring.finish()
    for out in outs:
        out.wait()
    for owner in range(n):
        for half in range(2):
            put(owner, half).wait()


def fused_body(n, tps, *args):
    x, cot, _, fac, _, first, _, _, _, weight, _ = args
    bf16, f32 = jnp.bfloat16, jnp.float32
    rows, rank = fac.shape
    width = cot.shape[1]
    rank_rows = first.shape[0]
    matrix = jax.ShapeDtypeStruct((rows, width), f32)
    copy = jax.ShapeDtypeStruct((rows * n, width), bf16)
    moment = jax.ShapeDtypeStruct((rank_rows, width), f32)
    dma = pltpu.SemaphoreType.DMA
    return pl.pallas_call(
        functools.partial(fused, n, tps),
        out_shape=(matrix, matrix, copy, moment, moment) * 2,
        in_specs=[ANY] * 11,
        out_specs=(ANY,) * 10,
        scratch_shapes=[
            pltpu.VMEM(x.shape, bf16),
            pltpu.VMEM((2,) + cot.shape, bf16),
            pltpu.VMEM((2,) + fac.shape, bf16),
            pltpu.VMEM((2,) + first.shape, f32),
            pltpu.VMEM((2,) + first.shape, f32),
            pltpu.VMEM((2, rows, width), f32),
            pltpu.VMEM((n,) + fac.shape, bf16),
            pltpu.VMEM((2, x.shape[0], rank), f32),
            pltpu.VMEM((n, 2) + first.shape, f32),
            pltpu.VMEM((n, 2) + first.shape, f32),
            pltpu.VMEM((n, 2) + first.shape, f32),
            pltpu.VMEM((tps, 2, 8, width), f32),
            pltpu.VMEM((2, rows, width), f32),
            pltpu.VMEM((2, rows, width), f32),
            pltpu.VMEM((n, 2, rows, width), bf16),
            dma((11,)),
            dma((8,)),
            dma((n, 2)),
            dma((2, n // 2, 2)),
            dma((2, n // 2, 2)),
            dma((2, n // 2, 2)),
            dma((2, n // 2, 2)),
            dma,
            dma,
            dma((n - 1,)),
            dma((n - 1,)),
            dma((n - 1,)),
            dma((n - 1,)),
            dma((tps - 1,)),
            dma((tps - 1,)),
        ],
        compiler_params=pltpu.CompilerParams(collective_id=0, has_side_effects=True),
    )(*args)


def split_three(values):
    upper = lax.optimization_barrier(values.astype(jnp.bfloat16))
    rest = values - upper.astype(jnp.float32)
    middle = lax.optimization_barrier(rest.astype(jnp.bfloat16))
    lower = (rest - middle.astype(jnp.float32)).astype(jnp.bfloat16)
    return (upper, middle, lower)


def project_tokens(mixed, cotangent):
    contract = (((0,), (0,)), ((), ()))
    total = jnp.zeros((mixed.shape[1], cotangent.shape[1]), jnp.float32)
    for piece in split_three(mixed):
        total = total + lax.dot_general(
            piece, cotangent, contract, preferred_element_type=jnp.float32
        )
    return total


def plain_body(
    block_input,
    query_cotangent,
    key_cotangent,
    query_factor,
    key_factor,
    query_first,
    query_second,
    key_first,
    key_second,
    query_weight,
    key_weight,
):
    query_wide = query_factor.astype(jnp.float32)
    key_wide = key_factor.astype(jnp.float32)
    whole_query, whole_key = (
        lax.all_gather(query_factor, "fs", axis=0, tiled=True),
        lax.all_gather(key_factor, "fs", axis=0, tiled=True),
    )
    mixed_query = jnp.dot(block_input, whole_query, preferred_element_type=jnp.float32)
    mixed_key = jnp.dot(block_input, whole_key, preferred_element_type=jnp.float32)
    query_part = project_tokens(mixed_query, query_cotangent)
    key_part = project_tokens(mixed_key, key_cotangent)
    small_query, small_key = (
        lax.psum_scatter(query_part, "fs", scatter_dimension=0, tiled=True),
        lax.psum_scatter(key_part, "fs", scatter_dimension=0, tiled=True),
    )
    query_first_new, query_second_new, query_direction = moments(
        small_query, query_first, query_second
    )
    key_first_new, key_second_new, key_direction = moments(small_key, key_first, key_second)
    full_query, full_key = (
        lax.all_gather(query_direction, "fs", axis=0, tiled=True),
        lax.all_gather(key_direction, "fs", axis=0, tiled=True),
    )
    query_square, key_square = lax.psum(
        (jnp.sum(query_direction * query_direction), jnp.sum(key_direction * key_direction)),
        ("fs", "tp"),
    )
    entry_count = full_query.shape[0] * full_query.shape[1] * lax.axis_size("tp")
    query_scale = 1.0 / jnp.maximum(jnp.sqrt(query_square / entry_count), scale_floor)
    key_scale = 1.0 / jnp.maximum(jnp.sqrt(key_square / entry_count), scale_floor)
    query_update = -query_scale * jnp.dot(query_wide, full_query, precision=lax.Precision.HIGHEST)
    key_update = -key_scale * jnp.dot(key_wide, full_key, precision=lax.Precision.HIGHEST)
    query_new = query_weight + learn_rate * query_update
    key_new = key_weight + learn_rate * key_update
    query_copy, key_copy = (
        lax.all_gather(query_new.astype(jnp.bfloat16), "fs", axis=0, tiled=True),
        lax.all_gather(key_new.astype(jnp.bfloat16), "fs", axis=0, tiled=True),
    )
    return (
        query_update,
        query_new,
        query_copy,
        query_first_new,
        query_second_new,
        key_update,
        key_new,
        key_copy,
        key_first_new,
        key_second_new,
    )


def solution(mesh):
    n, tps = mesh.shape["fs"], mesh.shape["tp"]
    split = P("fs", "tp")
    in_specs = (P("fs", None), split, split, P("fs", None), P("fs", None)) + (split,) * 6
    out_specs = (split, split, P(None, "tp"), split, split) * 2

    def body(*args):
        factor, first = args[3], args[5]
        whole_tiles = first.shape[0] % 8 == 0 and factor.shape[0] % 128 == 0
        if n % 2 == 0 and tps % 2 == 0 and whole_tiles:
            return fused_body(n, tps, *args)
        return plain_body(*args)

    return jax.shard_map(body, mesh=mesh, in_specs=in_specs, out_specs=out_specs, check_vma=False)
```

```python
import functools

import jax
import jax.numpy as jnp
from jax import lax
from jax.experimental import pallas as pl
from jax.experimental.pallas import tpu as pltpu
from jax.sharding import PartitionSpec as P

beta_one = 0.9
beta_two = 0.99
denom_floor = 0.001
scale_floor = 0.5
learn_rate = 0.02
MESH = pl.DeviceIdType.MESH
VMEM_GRANT = 24 * 1024 * 1024
SMALL_GRANT = 1024 * 1024
ANY = pl.BlockSpec(memory_space=pl.ANY)


def moments(small, first, second):
    first_new = beta_one * first + (1.0 - beta_one) * small
    second_new = beta_two * second + (1.0 - beta_two) * small * small
    direction = first_new / (jnp.sqrt(second_new) + denom_floor)
    return (first_new, second_new, direction)


def split_two(values):
    upper = values.astype(jnp.bfloat16)
    lower = (values - upper.astype(jnp.float32)).astype(jnp.bfloat16)
    return (upper, lower)


def ring_place(index, n):
    odd = index % 2
    along = index // 2
    return (1 - odd) * along + odd * (n - 1 - along)


def ring_index(place, n):
    back = place // (n // 2)
    return (1 - back) * (2 * place) + back * (2 * (n - 1 - place) + 1)


class Ring:
    def __init__(self, n, me, own, slot, send, recv):
        self.n, self.own, self.slot, self.send, self.recv = n, own, slot, send, recv
        self.me = me
        self.place = ring_place(me, n)
        self.last = n // 2

    def active(self, step, way, half):
        return step < self.last or (step == self.last and way == half)

    def owner(self, step, way):
        shift = -step if way == 0 else step
        return ring_index((self.place + shift + self.n) % self.n, self.n)

    def copy(self, step, way, half):
        shift = 1 if way == 0 else self.n - 1
        to = ring_index((self.place + shift) % self.n, self.n)
        if step == 1:
            owner, src = self.me, self.own(half)
        else:
            owner = self.owner(step - 1, way)
            src = self.slot(owner, half)
        return pltpu.make_async_remote_copy(
            src_ref=src,
            dst_ref=self.slot(owner, half),
            send_sem=self.send.at[way, step - 1, half],
            recv_sem=self.recv.at[way, step - 1, half],
            device_id={"fs": to},
            device_id_type=MESH,
        )

    def begin(self, half):
        for way in range(2):
            if self.active(1, way, half):
                self.copy(1, way, half).start()

    def step(self, step, arrived):
        for half in range(2):
            for way in range(2):
                if self.active(step, way, half):
                    self.copy(step, way, half).wait_recv()
                    if self.active(step + 1, way, half):
                        self.copy(step + 1, way, half).start()
                    arrived(self.owner(step, way), half)

    def finish(self):
        for step in range(1, self.last + 1):
            for way in range(2):
                for half in range(2):
                    if self.active(step, way, half):
                        self.copy(step, way, half).wait_send()


def fused(
    n,
    tps,
    x_in,
    cq_in,
    ck_in,
    fq_in,
    fk_in,
    q1_in,
    q2_in,
    k1_in,
    k2_in,
    wq_in,
    wk_in,
    uq_out,
    nq_out,
    cq_out,
    q1_out,
    q2_out,
    uk_out,
    nk_out,
    ck_out,
    k1_out,
    k2_out,
    x,
    cot,
    fac,
    first,
    second,
    weight,
    gathered,
    mix,
    part,
    near,
    paired,
    far,
    dirs,
    squares,
    update,
    in_sem,
    ring_a_send,
    ring_a_recv,
    ring_e_send,
    ring_e_recv,
    mix_send,
    mix_recv,
    near_send,
    near_recv,
    far_send,
    far_recv,
    dir_send,
    dir_recv,
    pass_send,
    pass_recv,
    sq_send,
    sq_recv,
):
    me = lax.axis_index("fs")
    tp = lax.axis_index("tp")
    core = tp % 2
    rows = fac.shape[1]
    half_rows = rows // 2
    rank_rows = first.shape[1]
    rank = n * rank_rows
    width = cot.shape[2]
    planes = n // 2
    side = me % 2
    plane = me // 2
    twin = me + 1 - 2 * side
    copies = (cq_out, ck_out)
    update_outs = (uq_out, uk_out)
    new_outs = (nq_out, nk_out)
    first_outs = (q1_out, k1_out)
    second_outs = (q2_out, k2_out)

    loads = [
        pltpu.make_async_copy(src, dst, in_sem.at[i])
        for i, (src, dst) in enumerate(
            (
                (fq_in, fac.at[0]),
                (fk_in, fac.at[1]),
                (x_in, x),
                (cq_in, cot.at[0]),
                (ck_in, cot.at[1]),
                (q1_in, first.at[0]),
                (k1_in, first.at[1]),
                (q2_in, second.at[0]),
                (k2_in, second.at[1]),
                (wq_in, weight.at[0]),
                (wk_in, weight.at[1]),
            )
        )
    ]
    for load in loads:
        load.start()

    barrier = pltpu.get_barrier_semaphore()
    for k in range(1, n):
        pl.semaphore_signal(barrier, inc=1, device_id={"fs": (me + k) % n}, device_id_type=MESH)
    for k in range(1, tps):
        pl.semaphore_signal(barrier, inc=1, device_id={"tp": (tp + k) % tps}, device_id_type=MESH)
    pl.semaphore_wait(barrier, n + tps - 2)

    loads[0].wait()
    loads[1].wait()
    ring = Ring(
        n,
        me,
        lambda half: fac.at[core, pl.ds(half * half_rows, half_rows)],
        lambda owner, half: gathered.at[owner, pl.ds(half * half_rows, half_rows)],
        ring_a_send,
        ring_a_recv,
    )
    ring.begin(0)
    ring.begin(1)
    loads[2].wait()

    def product(owner, block):
        columns = pl.ds(pl.multiple_of(owner * rows, 128), rows)
        return jnp.dot(x[:, columns], block, preferred_element_type=jnp.float32)

    mixed = product(me, fac[core])
    for step in range(1, planes + 1):
        ring.step(step, lambda owner, half: None)
        for way in range(2 if step < planes else 1):
            owner = ring.owner(step, way)
            mixed += product(owner, gathered[owner])
    mix[core] = mixed

    swap = pltpu.make_async_remote_copy(
        src_ref=mix.at[core],
        dst_ref=mix.at[core],
        send_sem=mix_send,
        recv_sem=mix_recv,
        device_id={"tp": tp + 1 - 2 * core},
        device_id_type=MESH,
    )
    swap.start()
    for load in loads[3:]:
        load.wait()
    swap.wait()

    def to_near(p, k):
        to = (plane + k) % planes
        return pltpu.make_async_remote_copy(
            src_ref=part.at[p, 2 * to + 1 - side],
            dst_ref=near.at[p, to],
            send_sem=near_send.at[p, k],
            recv_sem=near_recv.at[p, k],
            device_id={"fs": twin},
            device_id_type=MESH,
        )

    def to_far(p, k):
        to = (plane + k) % planes
        return pltpu.make_async_remote_copy(
            src_ref=paired.at[p, to],
            dst_ref=far.at[p, plane],
            send_sem=far_send.at[p, k],
            recv_sem=far_recv.at[p, k],
            device_id={"fs": 2 * to + side},
            device_id_type=MESH,
        )

    order = tuple(range(1, planes)) + (0,)
    contract = (((0,), (0,)), ((), ()))
    for p in range(2):
        upper, lower = split_two(mix[p])
        total = lax.dot_general(upper, cot[p], contract, preferred_element_type=jnp.float32)
        total += lax.dot_general(lower, cot[p], contract, preferred_element_type=jnp.float32)
        part[p] = total.reshape(n, rank_rows, width)
        for k in order:
            to_near(p, k).start()
    for p in range(2):
        for k in order:
            to_near(p, k).wait_recv()
            to = (plane + k) % planes
            paired[p, to] = part[p, 2 * to + side] + near[p, to]
            if k:
                to_far(p, k).start()

    def spread(p, k):
        if k == 0:
            to = twin
        else:
            to = 2 * ((plane + k) % planes) + side
        return pltpu.make_async_remote_copy(
            src_ref=dirs.at[p, me],
            dst_ref=dirs.at[p, me],
            send_sem=dir_send.at[p, k],
            recv_sem=dir_recv.at[p, k],
            device_id={"fs": to},
            device_id_type=MESH,
        )

    def hand_on(p, k):
        owner = 2 * ((plane - k + planes) % planes) + side
        return pltpu.make_async_remote_copy(
            src_ref=dirs.at[p, owner],
            dst_ref=dirs.at[p, owner],
            send_sem=pass_send.at[p, k - 1],
            recv_sem=pass_recv.at[p, k - 1],
            device_id={"fs": twin},
            device_id_type=MESH,
        )

    def tell(p, k):
        return pltpu.make_async_remote_copy(
            src_ref=squares.at[p, tp],
            dst_ref=squares.at[p, tp],
            send_sem=sq_send.at[p, k - 1],
            recv_sem=sq_recv.at[p, k - 1],
            device_id={"tp": (tp + k) % tps},
            device_id_type=MESH,
        )

    for p in range(2):
        small = paired[p, plane]
        for k in range(1, planes):
            to_far(p, k).wait_recv()
            small += far[p, (plane - k + planes) % planes]
        first_new, second_new, direction = moments(small, first[p], second[p])
        dirs[p, me] = direction
        for k in order:
            spread(p, k).start()
        first_outs[p][...] = first_new
        second_outs[p][...] = second_new

    for p in range(2):
        for k in range(1, planes):
            spread(p, k).wait_recv()
            hand_on(p, k).start()
    for p in range(2):
        spread(p, 0).wait_recv()
        for k in range(1, planes):
            hand_on(p, k).wait_recv()
        full = dirs[p].reshape(rank, width)
        squares[p, tp] = jnp.sum((full * full).reshape(rank // 8, 8, width), axis=0)
        for k in range(1, tps):
            tell(p, k).start()
        upper, lower = split_two(full)
        total = jnp.dot(fac[p], upper, preferred_element_type=jnp.float32)
        update[p] = total + jnp.dot(fac[p], lower, preferred_element_type=jnp.float32)

    def block(owner, half):
        return copies[half].at[pl.ds(pl.multiple_of(owner * rows, 128), rows)]

    outer = Ring(n, me, lambda half: block(me, half), block, ring_e_send, ring_e_recv)
    for p in range(2):
        for k in range(1, tps):
            tell(p, k).wait_recv()
        square = jnp.sum(jnp.sum(squares[p], axis=0), keepdims=True)
        scale = 1.0 / jnp.maximum(jnp.sqrt(square / (rank * width * tps)), scale_floor)
        step = -scale * update[p]
        made = weight[p] + learn_rate * step
        block(me, p)[...] = made.astype(jnp.bfloat16)
        outer.begin(p)
        update_outs[p][...] = step
        new_outs[p][...] = made

    for step in range(1, planes + 1):
        outer.step(step, lambda owner, half: None)
    ring.finish()
    for p in range(2):
        for k in order:
            to_near(p, k).wait_send()
            spread(p, k).wait_send()
            if k:
                to_far(p, k).wait_send()
                hand_on(p, k).wait_send()
        for k in range(1, tps):
            tell(p, k).wait_send()
    outer.finish()


def settle(count, *refs):
    sems = refs[2 * count]
    moves = []
    for i in range(count):
        moves.append(pltpu.make_async_copy(refs[i], refs[count + i], sems.at[i]))
    for move in moves:
        move.start()
    for move in moves:
        move.wait()


def fused_body(n, tps, *args):
    x, cot, _, fac, _, first, _, _, _, weight, _ = args
    bf16, f32 = jnp.bfloat16, jnp.float32
    rows, rank = fac.shape
    width = cot.shape[1]
    rank_rows = first.shape[0]
    planes = n // 2
    matrix = jax.ShapeDtypeStruct((rows, width), f32)
    copy = jax.ShapeDtypeStruct((rows * n, width), bf16)
    moment = jax.ShapeDtypeStruct((rank_rows, width), f32)
    outs = (matrix, matrix, copy, moment, moment) * 2
    dma = pltpu.SemaphoreType.DMA
    vmem = pltpu.VMEM
    made = pl.pallas_call(
        functools.partial(fused, n, tps),
        out_shape=outs,
        in_specs=[pl.BlockSpec(memory_space=pltpu.HBM)] * 11,
        out_specs=(pl.BlockSpec(memory_space=pltpu.VMEM),) * 10,
        scratch_shapes=[
            vmem(x.shape, bf16),
            vmem((2,) + cot.shape, bf16),
            vmem((2,) + fac.shape, bf16),
            vmem((2,) + first.shape, f32),
            vmem((2,) + first.shape, f32),
            vmem((2, rows, width), f32),
            vmem((n,) + fac.shape, bf16),
            vmem((2, x.shape[0], rank), f32),
            vmem((2, n) + first.shape, f32),
            vmem((2, planes) + first.shape, f32),
            vmem((2, planes) + first.shape, f32),
            vmem((2, planes) + first.shape, f32),
            vmem((2, n) + first.shape, f32),
            vmem((2, tps, 8, width), f32),
            vmem((2, rows, width), f32),
            dma((11,)),
            dma((2, planes, 2)),
            dma((2, planes, 2)),
            dma((2, planes, 2)),
            dma((2, planes, 2)),
            dma,
            dma,
            dma((2, planes)),
            dma((2, planes)),
            dma((2, planes)),
            dma((2, planes)),
            dma((2, planes)),
            dma((2, planes)),
            dma((2, planes - 1)),
            dma((2, planes - 1)),
            dma((2, tps - 1)),
            dma((2, tps - 1)),
        ],
        compiler_params=pltpu.CompilerParams(
            collective_id=0, has_side_effects=True, vmem_limit_bytes=VMEM_GRANT
        ),
    )(*args)
    return pl.pallas_call(
        functools.partial(settle, len(outs)),
        out_shape=outs,
        in_specs=[ANY] * len(outs),
        out_specs=(ANY,) * len(outs),
        scratch_shapes=[dma((len(outs),))],
        compiler_params=pltpu.CompilerParams(vmem_limit_bytes=SMALL_GRANT),
    )(*made)


def split_three(values):
    upper = lax.optimization_barrier(values.astype(jnp.bfloat16))
    rest = values - upper.astype(jnp.float32)
    middle = lax.optimization_barrier(rest.astype(jnp.bfloat16))
    lower = (rest - middle.astype(jnp.float32)).astype(jnp.bfloat16)
    return (upper, middle, lower)


def project_tokens(mixed, cotangent):
    contract = (((0,), (0,)), ((), ()))
    total = jnp.zeros((mixed.shape[1], cotangent.shape[1]), jnp.float32)
    for piece in split_three(mixed):
        total = total + lax.dot_general(
            piece, cotangent, contract, preferred_element_type=jnp.float32
        )
    return total


def plain_body(
    block_input,
    query_cotangent,
    key_cotangent,
    query_factor,
    key_factor,
    query_first,
    query_second,
    key_first,
    key_second,
    query_weight,
    key_weight,
):
    query_wide = query_factor.astype(jnp.float32)
    key_wide = key_factor.astype(jnp.float32)
    whole_query, whole_key = (
        lax.all_gather(query_factor, "fs", axis=0, tiled=True),
        lax.all_gather(key_factor, "fs", axis=0, tiled=True),
    )
    mixed_query = jnp.dot(block_input, whole_query, preferred_element_type=jnp.float32)
    mixed_key = jnp.dot(block_input, whole_key, preferred_element_type=jnp.float32)
    query_part = project_tokens(mixed_query, query_cotangent)
    key_part = project_tokens(mixed_key, key_cotangent)
    small_query, small_key = (
        lax.psum_scatter(query_part, "fs", scatter_dimension=0, tiled=True),
        lax.psum_scatter(key_part, "fs", scatter_dimension=0, tiled=True),
    )
    query_first_new, query_second_new, query_direction = moments(
        small_query, query_first, query_second
    )
    key_first_new, key_second_new, key_direction = moments(small_key, key_first, key_second)
    full_query, full_key = (
        lax.all_gather(query_direction, "fs", axis=0, tiled=True),
        lax.all_gather(key_direction, "fs", axis=0, tiled=True),
    )
    query_square, key_square = lax.psum(
        (jnp.sum(query_direction * query_direction), jnp.sum(key_direction * key_direction)),
        ("fs", "tp"),
    )
    entry_count = full_query.shape[0] * full_query.shape[1] * lax.axis_size("tp")
    query_scale = 1.0 / jnp.maximum(jnp.sqrt(query_square / entry_count), scale_floor)
    key_scale = 1.0 / jnp.maximum(jnp.sqrt(key_square / entry_count), scale_floor)
    query_update = -query_scale * jnp.dot(query_wide, full_query, precision=lax.Precision.HIGHEST)
    key_update = -key_scale * jnp.dot(key_wide, full_key, precision=lax.Precision.HIGHEST)
    query_new = query_weight + learn_rate * query_update
    key_new = key_weight + learn_rate * key_update
    query_copy, key_copy = (
        lax.all_gather(query_new.astype(jnp.bfloat16), "fs", axis=0, tiled=True),
        lax.all_gather(key_new.astype(jnp.bfloat16), "fs", axis=0, tiled=True),
    )
    return (
        query_update,
        query_new,
        query_copy,
        query_first_new,
        query_second_new,
        key_update,
        key_new,
        key_copy,
        key_first_new,
        key_second_new,
    )


def solution(mesh):
    n, tps = mesh.shape["fs"], mesh.shape["tp"]
    split = P("fs", "tp")
    in_specs = (P("fs", None), split, split, P("fs", None), P("fs", None)) + (split,) * 6
    out_specs = (split, split, P(None, "tp"), split, split) * 2

    def body(*args):
        factor, first = args[3], args[5]
        whole_tiles = first.shape[0] % 8 == 0 and factor.shape[0] % 128 == 0
        if n % 2 == 0 and tps % 2 == 0 and whole_tiles:
            return fused_body(n, tps, *args)
        return plain_body(*args)

    return jax.shard_map(body, mesh=mesh, in_specs=in_specs, out_specs=out_specs, check_vma=False)
```

```python
import functools

import jax
import jax.numpy as jnp
from jax import lax
from jax.experimental import pallas as pl
from jax.experimental.pallas import tpu as pltpu
from jax.sharding import PartitionSpec as P

beta_one = 0.9
beta_two = 0.99
denom_floor = 0.001
scale_floor = 0.5
learn_rate = 0.02
MESH = pl.DeviceIdType.MESH
VMEM_GRANT = 24 * 1024 * 1024
SMALL_GRANT = 1024 * 1024
ANY = pl.BlockSpec(memory_space=pl.ANY)


def moments(small, first, second):
    first_new = beta_one * first + (1.0 - beta_one) * small
    second_new = beta_two * second + (1.0 - beta_two) * small * small
    direction = first_new / (jnp.sqrt(second_new) + denom_floor)
    return (first_new, second_new, direction)


def split_two(values):
    upper = values.astype(jnp.bfloat16)
    lower = (values - upper.astype(jnp.float32)).astype(jnp.bfloat16)
    return (upper, lower)


def ring_place(index, n):
    odd = index % 2
    along = index // 2
    return (1 - odd) * along + odd * (n - 1 - along)


def ring_index(place, n):
    back = place // (n // 2)
    return (1 - back) * (2 * place) + back * (2 * (n - 1 - place) + 1)


class Ring:
    def __init__(self, n, me, own, slot, send, recv):
        self.n, self.own, self.slot, self.send, self.recv = n, own, slot, send, recv
        self.me = me
        self.place = ring_place(me, n)
        self.last = n // 2

    def active(self, step, way, half):
        return step < self.last or (step == self.last and way == half)

    def owner(self, step, way):
        shift = -step if way == 0 else step
        return ring_index((self.place + shift + self.n) % self.n, self.n)

    def copy(self, step, way, half):
        shift = 1 if way == 0 else self.n - 1
        to = ring_index((self.place + shift) % self.n, self.n)
        if step == 1:
            owner, src = self.me, self.own(half)
        else:
            owner = self.owner(step - 1, way)
            src = self.slot(owner, half)
        return pltpu.make_async_remote_copy(
            src_ref=src,
            dst_ref=self.slot(owner, half),
            send_sem=self.send.at[way, step - 1, half],
            recv_sem=self.recv.at[way, step - 1, half],
            device_id={"fs": to},
            device_id_type=MESH,
        )

    def begin(self, half):
        for way in range(2):
            if self.active(1, way, half):
                self.copy(1, way, half).start()

    def step(self, step, arrived):
        for half in range(2):
            for way in range(2):
                if self.active(step, way, half):
                    self.copy(step, way, half).wait_recv()
                    if self.active(step + 1, way, half):
                        self.copy(step + 1, way, half).start()
                    arrived(self.owner(step, way), half)

    def finish(self):
        for step in range(1, self.last + 1):
            for way in range(2):
                for half in range(2):
                    if self.active(step, way, half):
                        self.copy(step, way, half).wait_send()


def fused(
    n,
    tps,
    x_in,
    cq_in,
    ck_in,
    fq_in,
    fk_in,
    q1_in,
    q2_in,
    k1_in,
    k2_in,
    wq_in,
    wk_in,
    uq_out,
    nq_out,
    cq_out,
    q1_out,
    q2_out,
    uk_out,
    nk_out,
    ck_out,
    k1_out,
    k2_out,
    x,
    cot,
    fac,
    first,
    second,
    weight,
    gathered,
    mix,
    part,
    near,
    paired,
    far,
    dirs,
    squares,
    update,
    in_sem,
    ring_a_send,
    ring_a_recv,
    ring_e_send,
    ring_e_recv,
    mix_send,
    mix_recv,
    near_send,
    near_recv,
    far_send,
    far_recv,
    dir_send,
    dir_recv,
    pass_send,
    pass_recv,
    sq_send,
    sq_recv,
):
    me = lax.axis_index("fs")
    tp = lax.axis_index("tp")
    core = tp % 2
    rows = fac.shape[1]
    half_rows = rows // 2
    rank_rows = first.shape[1]
    rank = n * rank_rows
    width = cot.shape[2]
    planes = n // 2
    side = me % 2
    plane = me // 2
    twin = me + 1 - 2 * side
    copies = (cq_out, ck_out)
    update_outs = (uq_out, uk_out)
    new_outs = (nq_out, nk_out)
    first_outs = (q1_out, k1_out)
    second_outs = (q2_out, k2_out)

    loads = [
        pltpu.make_async_copy(src, dst, in_sem.at[i])
        for i, (src, dst) in enumerate(
            (
                (fq_in, fac.at[0]),
                (fk_in, fac.at[1]),
                (x_in, x),
                (cq_in, cot.at[0]),
                (ck_in, cot.at[1]),
                (q1_in, first.at[0]),
                (k1_in, first.at[1]),
                (q2_in, second.at[0]),
                (k2_in, second.at[1]),
                (wq_in, weight.at[0]),
                (wk_in, weight.at[1]),
            )
        )
    ]
    for load in loads:
        load.start()

    barrier = pltpu.get_barrier_semaphore()
    for k in range(1, n):
        pl.semaphore_signal(barrier, inc=1, device_id={"fs": (me + k) % n}, device_id_type=MESH)
    for k in range(1, tps):
        pl.semaphore_signal(barrier, inc=1, device_id={"tp": (tp + k) % tps}, device_id_type=MESH)
    pl.semaphore_wait(barrier, n + tps - 2)

    loads[0].wait()
    loads[1].wait()
    ring = Ring(
        n,
        me,
        lambda half: fac.at[core, pl.ds(half * half_rows, half_rows)],
        lambda owner, half: gathered.at[owner, pl.ds(half * half_rows, half_rows)],
        ring_a_send,
        ring_a_recv,
    )
    ring.begin(0)
    ring.begin(1)
    loads[2].wait()

    def product(owner, block):
        columns = pl.ds(pl.multiple_of(owner * rows, 128), rows)
        return jnp.dot(x[:, columns], block, preferred_element_type=jnp.float32)

    mixed = product(me, fac[core])
    for step in range(1, planes + 1):
        ring.step(step, lambda owner, half: None)
        for way in range(2 if step < planes else 1):
            owner = ring.owner(step, way)
            mixed += product(owner, gathered[owner])
    mix[core] = mixed

    swap = pltpu.make_async_remote_copy(
        src_ref=mix.at[core],
        dst_ref=mix.at[core],
        send_sem=mix_send,
        recv_sem=mix_recv,
        device_id={"tp": tp + 1 - 2 * core},
        device_id_type=MESH,
    )
    swap.start()
    for load in loads[3:]:
        load.wait()
    swap.wait()

    def to_near(p, k):
        to = (plane + k) % planes
        return pltpu.make_async_remote_copy(
            src_ref=part.at[p, 2 * to + 1 - side],
            dst_ref=near.at[p, to],
            send_sem=near_send.at[p, k],
            recv_sem=near_recv.at[p, k],
            device_id={"fs": twin},
            device_id_type=MESH,
        )

    def to_far(p, k):
        to = (plane + k) % planes
        return pltpu.make_async_remote_copy(
            src_ref=paired.at[p, to],
            dst_ref=far.at[p, plane],
            send_sem=far_send.at[p, k],
            recv_sem=far_recv.at[p, k],
            device_id={"fs": 2 * to + side},
            device_id_type=MESH,
        )

    order = tuple(range(1, planes)) + (0,)
    contract = (((0,), (0,)), ((), ()))
    for p in range(2):
        upper, lower = split_two(mix[p])
        total = lax.dot_general(upper, cot[p], contract, preferred_element_type=jnp.float32)
        total += lax.dot_general(lower, cot[p], contract, preferred_element_type=jnp.float32)
        part[p] = total.reshape(n, rank_rows, width)
        for k in order:
            to_near(p, k).start()
    for p in range(2):
        for k in order:
            to_near(p, k).wait_recv()
            to = (plane + k) % planes
            paired[p, to] = part[p, 2 * to + side] + near[p, to]
            if k:
                to_far(p, k).start()

    def spread(p, k):
        if k == 0:
            to = twin
        else:
            to = 2 * ((plane + k) % planes) + side
        return pltpu.make_async_remote_copy(
            src_ref=dirs.at[p, me],
            dst_ref=dirs.at[p, me],
            send_sem=dir_send.at[p, k],
            recv_sem=dir_recv.at[p, k],
            device_id={"fs": to},
            device_id_type=MESH,
        )

    def hand_on(p, k):
        owner = 2 * ((plane - k + planes) % planes) + side
        return pltpu.make_async_remote_copy(
            src_ref=dirs.at[p, owner],
            dst_ref=dirs.at[p, owner],
            send_sem=pass_send.at[p, k - 1],
            recv_sem=pass_recv.at[p, k - 1],
            device_id={"fs": twin},
            device_id_type=MESH,
        )

    def tell(p, k):
        return pltpu.make_async_remote_copy(
            src_ref=squares.at[p, tp],
            dst_ref=squares.at[p, tp],
            send_sem=sq_send.at[p, k - 1],
            recv_sem=sq_recv.at[p, k - 1],
            device_id={"tp": (tp + k) % tps},
            device_id_type=MESH,
        )

    for p in range(2):
        small = paired[p, plane]
        for k in range(1, planes):
            to_far(p, k).wait_recv()
            small += far[p, (plane - k + planes) % planes]
        first_new, second_new, direction = moments(small, first[p], second[p])
        dirs[p, me] = direction
        for k in order:
            spread(p, k).start()
        first_outs[p][...] = first_new
        second_outs[p][...] = second_new

    for p in range(2):
        for k in range(1, planes):
            spread(p, k).wait_recv()
            hand_on(p, k).start()
    for p in range(2):
        spread(p, 0).wait_recv()
        for k in range(1, planes):
            hand_on(p, k).wait_recv()
        full = dirs[p].reshape(rank, width)
        squares[p, tp] = jnp.sum((full * full).reshape(rank // 8, 8, width), axis=0)
        for k in range(1, tps):
            tell(p, k).start()
        upper, lower = split_two(full)
        total = jnp.dot(fac[p], upper, preferred_element_type=jnp.float32)
        update[p] = total + jnp.dot(fac[p], lower, preferred_element_type=jnp.float32)

    def block(owner, half):
        return copies[half].at[pl.ds(pl.multiple_of(owner * rows, 128), rows)]

    outer = Ring(n, me, lambda half: block(me, half), block, ring_e_send, ring_e_recv)
    for p in range(2):
        for k in range(1, tps):
            tell(p, k).wait_recv()
        square = jnp.sum(jnp.sum(squares[p], axis=0), keepdims=True)
        scale = 1.0 / jnp.maximum(jnp.sqrt(square / (rank * width * tps)), scale_floor)
        step = -scale * update[p]
        made = weight[p] + learn_rate * step
        block(me, p)[...] = made.astype(jnp.bfloat16)
        outer.begin(p)
        update_outs[p][...] = step
        new_outs[p][...] = made

    for step in range(1, planes + 1):
        outer.step(step, lambda owner, half: None)
    ring.finish()
    for p in range(2):
        for k in order:
            to_near(p, k).wait_send()
            spread(p, k).wait_send()
            if k:
                to_far(p, k).wait_send()
                hand_on(p, k).wait_send()
        for k in range(1, tps):
            tell(p, k).wait_send()
    outer.finish()


def settle(count, *refs):
    sems = refs[2 * count]
    moves = []
    for i in range(count):
        moves.append(pltpu.make_async_copy(refs[i], refs[count + i], sems.at[i]))
    for move in moves:
        move.start()
    for move in moves:
        move.wait()


def fused_body(n, tps, *args):
    x, cot, _, fac, _, first, _, _, _, weight, _ = args
    bf16, f32 = jnp.bfloat16, jnp.float32
    rows, rank = fac.shape
    width = cot.shape[1]
    rank_rows = first.shape[0]
    planes = n // 2
    matrix = jax.ShapeDtypeStruct((rows, width), f32)
    copy = jax.ShapeDtypeStruct((rows * n, width), bf16)
    moment = jax.ShapeDtypeStruct((rank_rows, width), f32)
    outs = (matrix, matrix, copy, moment, moment) * 2
    dma = pltpu.SemaphoreType.DMA
    vmem = pltpu.VMEM
    made = pl.pallas_call(
        functools.partial(fused, n, tps),
        out_shape=outs,
        in_specs=[pl.BlockSpec(memory_space=pltpu.HBM)] * 11,
        out_specs=(pl.BlockSpec(memory_space=pltpu.VMEM),) * 10,
        scratch_shapes=[
            vmem(x.shape, bf16),
            vmem((2,) + cot.shape, bf16),
            vmem((2,) + fac.shape, bf16),
            vmem((2,) + first.shape, f32),
            vmem((2,) + first.shape, f32),
            vmem((2, rows, width), f32),
            vmem((n,) + fac.shape, bf16),
            vmem((2, x.shape[0], rank), f32),
            vmem((2, n) + first.shape, f32),
            vmem((2, planes) + first.shape, f32),
            vmem((2, planes) + first.shape, f32),
            vmem((2, planes) + first.shape, f32),
            vmem((2, n) + first.shape, f32),
            vmem((2, tps, 8, width), f32),
            vmem((2, rows, width), f32),
            dma((11,)),
            dma((2, planes, 2)),
            dma((2, planes, 2)),
            dma((2, planes, 2)),
            dma((2, planes, 2)),
            dma,
            dma,
            dma((2, planes)),
            dma((2, planes)),
            dma((2, planes)),
            dma((2, planes)),
            dma((2, planes)),
            dma((2, planes)),
            dma((2, planes - 1)),
            dma((2, planes - 1)),
            dma((2, tps - 1)),
            dma((2, tps - 1)),
        ],
        compiler_params=pltpu.CompilerParams(
            collective_id=0, has_side_effects=True, vmem_limit_bytes=VMEM_GRANT
        ),
    )(*[pltpu.with_memory_space_constraint(arg, pltpu.HBM) for arg in args])
    return pl.pallas_call(
        functools.partial(settle, len(outs)),
        out_shape=outs,
        in_specs=[ANY] * len(outs),
        out_specs=(ANY,) * len(outs),
        scratch_shapes=[dma((len(outs),))],
        compiler_params=pltpu.CompilerParams(vmem_limit_bytes=SMALL_GRANT),
    )(*made)


def split_three(values):
    upper = lax.optimization_barrier(values.astype(jnp.bfloat16))
    rest = values - upper.astype(jnp.float32)
    middle = lax.optimization_barrier(rest.astype(jnp.bfloat16))
    lower = (rest - middle.astype(jnp.float32)).astype(jnp.bfloat16)
    return (upper, middle, lower)


def project_tokens(mixed, cotangent):
    contract = (((0,), (0,)), ((), ()))
    total = jnp.zeros((mixed.shape[1], cotangent.shape[1]), jnp.float32)
    for piece in split_three(mixed):
        total = total + lax.dot_general(
            piece, cotangent, contract, preferred_element_type=jnp.float32
        )
    return total


def plain_body(
    block_input,
    query_cotangent,
    key_cotangent,
    query_factor,
    key_factor,
    query_first,
    query_second,
    key_first,
    key_second,
    query_weight,
    key_weight,
):
    query_wide = query_factor.astype(jnp.float32)
    key_wide = key_factor.astype(jnp.float32)
    whole_query, whole_key = (
        lax.all_gather(query_factor, "fs", axis=0, tiled=True),
        lax.all_gather(key_factor, "fs", axis=0, tiled=True),
    )
    mixed_query = jnp.dot(block_input, whole_query, preferred_element_type=jnp.float32)
    mixed_key = jnp.dot(block_input, whole_key, preferred_element_type=jnp.float32)
    query_part = project_tokens(mixed_query, query_cotangent)
    key_part = project_tokens(mixed_key, key_cotangent)
    small_query, small_key = (
        lax.psum_scatter(query_part, "fs", scatter_dimension=0, tiled=True),
        lax.psum_scatter(key_part, "fs", scatter_dimension=0, tiled=True),
    )
    query_first_new, query_second_new, query_direction = moments(
        small_query, query_first, query_second
    )
    key_first_new, key_second_new, key_direction = moments(small_key, key_first, key_second)
    full_query, full_key = (
        lax.all_gather(query_direction, "fs", axis=0, tiled=True),
        lax.all_gather(key_direction, "fs", axis=0, tiled=True),
    )
    query_square, key_square = lax.psum(
        (jnp.sum(query_direction * query_direction), jnp.sum(key_direction * key_direction)),
        ("fs", "tp"),
    )
    entry_count = full_query.shape[0] * full_query.shape[1] * lax.axis_size("tp")
    query_scale = 1.0 / jnp.maximum(jnp.sqrt(query_square / entry_count), scale_floor)
    key_scale = 1.0 / jnp.maximum(jnp.sqrt(key_square / entry_count), scale_floor)
    query_update = -query_scale * jnp.dot(query_wide, full_query, precision=lax.Precision.HIGHEST)
    key_update = -key_scale * jnp.dot(key_wide, full_key, precision=lax.Precision.HIGHEST)
    query_new = query_weight + learn_rate * query_update
    key_new = key_weight + learn_rate * key_update
    query_copy, key_copy = (
        lax.all_gather(query_new.astype(jnp.bfloat16), "fs", axis=0, tiled=True),
        lax.all_gather(key_new.astype(jnp.bfloat16), "fs", axis=0, tiled=True),
    )
    return (
        query_update,
        query_new,
        query_copy,
        query_first_new,
        query_second_new,
        key_update,
        key_new,
        key_copy,
        key_first_new,
        key_second_new,
    )


def solution(mesh):
    n, tps = mesh.shape["fs"], mesh.shape["tp"]
    split = P("fs", "tp")
    in_specs = (P("fs", None), split, split, P("fs", None), P("fs", None)) + (split,) * 6
    out_specs = (split, split, P(None, "tp"), split, split) * 2

    def body(*args):
        factor, first = args[3], args[5]
        whole_tiles = first.shape[0] % 8 == 0 and factor.shape[0] % 128 == 0
        if n % 2 == 0 and tps % 2 == 0 and whole_tiles:
            return fused_body(n, tps, *args)
        return plain_body(*args)

    return jax.shard_map(body, mesh=mesh, in_specs=in_specs, out_specs=out_specs, check_vma=False)
```

```python
import functools

import jax
import jax.numpy as jnp
from jax import lax
from jax.experimental import pallas as pl
from jax.experimental.pallas import tpu as pltpu
from jax.sharding import PartitionSpec as P

beta_one = 0.9
beta_two = 0.99
denom_floor = 0.001
scale_floor = 0.5
learn_rate = 0.02
MESH = pl.DeviceIdType.MESH
VMEM_GRANT = 24 * 1024 * 1024
SMALL_GRANT = 1024 * 1024
A_PIECES = 4
E_ROWS = 64
ANY = pl.BlockSpec(memory_space=pl.ANY)


def moments(small, first, second):
    first_new = beta_one * first + (1.0 - beta_one) * small
    second_new = beta_two * second + (1.0 - beta_two) * small * small
    direction = first_new / (jnp.sqrt(second_new) + denom_floor)
    return (first_new, second_new, direction)


def split_two(values):
    upper = values.astype(jnp.bfloat16)
    lower = (values - upper.astype(jnp.float32)).astype(jnp.bfloat16)
    return (upper, lower)


def ring_place(index, n):
    odd = index % 2
    along = index // 2
    return (1 - odd) * along + odd * (n - 1 - along)


def ring_index(place, n):
    back = place // (n // 2)
    return (1 - back) * (2 * place) + back * (2 * (n - 1 - place) + 1)


class Ring:
    def __init__(self, n, me, pieces, own, slot, send, recv):
        self.n, self.me, self.pieces = n, me, pieces
        self.own, self.slot, self.send, self.recv = own, slot, send, recv
        self.place = ring_place(me, n)
        self.last = n // 2

    def active(self, step, way, piece):
        return step < self.last or (step == self.last and way == piece % 2)

    def owner(self, step, way):
        shift = -step if way == 0 else step
        return ring_index((self.place + shift + self.n) % self.n, self.n)

    def copy(self, step, way, piece):
        shift = 1 if way == 0 else self.n - 1
        to = ring_index((self.place + shift) % self.n, self.n)
        if step == 1:
            owner, src = self.me, self.own(piece)
        else:
            owner = self.owner(step - 1, way)
            src = self.slot(owner, piece)
        return pltpu.make_async_remote_copy(
            src_ref=src,
            dst_ref=self.slot(owner, piece),
            send_sem=self.send.at[way, step - 1, piece],
            recv_sem=self.recv.at[way, step - 1, piece],
            device_id={"fs": to},
            device_id_type=MESH,
        )

    def begin(self, pieces):
        for piece in pieces:
            for way in range(2):
                if self.active(1, way, piece):
                    self.copy(1, way, piece).start()

    def step(self, step):
        for piece in range(self.pieces):
            for way in range(2):
                if self.active(step, way, piece):
                    self.copy(step, way, piece).wait_recv()
                    if self.active(step + 1, way, piece):
                        self.copy(step + 1, way, piece).start()

    def finish(self):
        for step in range(1, self.last + 1):
            for way in range(2):
                for piece in range(self.pieces):
                    if self.active(step, way, piece):
                        self.copy(step, way, piece).wait_send()


def fused(
    n,
    tps,
    x_in,
    cq_in,
    ck_in,
    fq_in,
    fk_in,
    q1_in,
    q2_in,
    k1_in,
    k2_in,
    wq_in,
    wk_in,
    update_out,
    new_out,
    copies,
    first_out,
    second_out,
    x,
    cot,
    fac,
    first,
    second,
    weight,
    gathered,
    mix,
    part,
    near,
    paired,
    far,
    dirs,
    squares,
    sums,
    in_sem,
    ring_a_send,
    ring_a_recv,
    ring_e_send,
    ring_e_recv,
    mix_send,
    mix_recv,
    near_send,
    near_recv,
    far_send,
    far_recv,
    dir_send,
    dir_recv,
    pass_send,
    pass_recv,
    sq_send,
    sq_recv,
):
    me = lax.axis_index("fs")
    tp = lax.axis_index("tp")
    core = tp % 2
    chains = (0, 1)
    rows = fac.shape[1]
    rank_rows = first.shape[1]
    rank = n * rank_rows
    width = cot.shape[2]
    planes = n // 2
    side = me % 2
    plane = me // 2
    twin = me + 1 - 2 * side

    loads = [
        pltpu.make_async_copy(src, dst, in_sem.at[i])
        for i, (src, dst) in enumerate(
            (
                (fq_in, fac.at[0]),
                (fk_in, fac.at[1]),
                (x_in, x),
                (cq_in, cot.at[0]),
                (ck_in, cot.at[1]),
                (wq_in, weight.at[0]),
                (wk_in, weight.at[1]),
                (q1_in, first.at[0]),
                (k1_in, first.at[1]),
                (q2_in, second.at[0]),
                (k2_in, second.at[1]),
            )
        )
    ]
    for load in loads:
        load.start()

    barrier = pltpu.get_barrier_semaphore()
    place = ring_place(me, n)
    for shift in (1, n - 1):
        to = ring_index((place + shift) % n, n)
        pl.semaphore_signal(barrier, inc=1, device_id={"fs": to}, device_id_type=MESH)
    for k in range(1, tps):
        pl.semaphore_signal(barrier, inc=1, device_id={"tp": (tp + k) % tps}, device_id_type=MESH)
    pl.semaphore_wait(barrier, 2 + tps - 1)

    loads[0].wait()
    loads[1].wait()
    cut = rows // A_PIECES
    ring = Ring(
        n,
        me,
        A_PIECES,
        lambda piece: fac.at[core, pl.ds(piece * cut, cut)],
        lambda owner, piece: gathered.at[owner, pl.ds(piece * cut, cut)],
        ring_a_send,
        ring_a_recv,
    )
    ring.begin(range(A_PIECES))
    loads[2].wait()

    def product(owner, block):
        columns = pl.ds(pl.multiple_of(owner * rows, 128), rows)
        return jnp.dot(x[:, columns], block, preferred_element_type=jnp.float32)

    mixed = product(me, fac[core])
    for step in range(1, planes):
        ring.step(step)
        for way in range(2):
            owner = ring.owner(step, way)
            mixed += product(owner, gathered[owner])
    loads[5].wait()
    loads[6].wait()
    ring.step(planes)
    owner = ring.owner(planes, 0)
    mix[core] = mixed + product(owner, gathered[owner])

    swap = pltpu.make_async_remote_copy(
        src_ref=mix.at[core],
        dst_ref=mix.at[core],
        send_sem=mix_send,
        recv_sem=mix_recv,
        device_id={"tp": tp + 1 - 2 * core},
        device_id_type=MESH,
    )
    swap.start()
    loads[3].wait()
    loads[4].wait()

    def to_near(p, c, k):
        to = (plane + k) % planes
        return pltpu.make_async_remote_copy(
            src_ref=part.at[c, 2 * to + 1 - side],
            dst_ref=near.at[c, to],
            send_sem=near_send.at[p, k],
            recv_sem=near_recv.at[p, k],
            device_id={"fs": twin},
            device_id_type=MESH,
        )

    def to_far(p, c, k):
        to = (plane + k) % planes
        return pltpu.make_async_remote_copy(
            src_ref=paired.at[c, to],
            dst_ref=far.at[c, plane],
            send_sem=far_send.at[p, k],
            recv_sem=far_recv.at[p, k],
            device_id={"fs": 2 * to + side},
            device_id_type=MESH,
        )

    order = tuple(range(1, planes)) + (0,)
    contract = (((0,), (0,)), ((), ()))
    for p, c in enumerate(chains):
        if p == 0:
            swap.wait()
        upper, lower = split_two(mix[c])
        total = lax.dot_general(upper, cot[c], contract, preferred_element_type=jnp.float32)
        total += lax.dot_general(lower, cot[c], contract, preferred_element_type=jnp.float32)
        part[c] = total.reshape(n, rank_rows, width)
        for k in order:
            to_near(p, c, k).start()
    for load in loads[7:]:
        load.wait()
    for p, c in enumerate(chains):
        for k in order:
            to_near(p, c, k).wait_recv()
            to = (plane + k) % planes
            paired[c, to] = part[c, 2 * to + side] + near[c, to]
            if k:
                to_far(p, c, k).start()

    def held(p, owner):
        return sums.at[p - 2, owner] if p >= 2 else dirs.at[p, owner]

    def spread(p, k):
        to = 2 * ((plane + k) % planes) + side if k else twin
        return pltpu.make_async_remote_copy(
            src_ref=held(p, me),
            dst_ref=held(p, me),
            send_sem=dir_send.at[p, k],
            recv_sem=dir_recv.at[p, k],
            device_id={"fs": to},
            device_id_type=MESH,
        )

    def hand_on(p, k):
        owner = 2 * ((plane - k + planes) % planes) + side
        return pltpu.make_async_remote_copy(
            src_ref=held(p, owner),
            dst_ref=held(p, owner),
            send_sem=pass_send.at[p, k - 1],
            recv_sem=pass_recv.at[p, k - 1],
            device_id={"fs": twin},
            device_id_type=MESH,
        )

    def tell(p, k):
        return pltpu.make_async_remote_copy(
            src_ref=squares.at[p, tp],
            dst_ref=squares.at[p, tp],
            send_sem=sq_send.at[p, k - 1],
            recv_sem=sq_recv.at[p, k - 1],
            device_id={"tp": (tp + k) % tps},
            device_id_type=MESH,
        )

    def move(p):
        small = paired[p, plane]
        for k in range(1, planes):
            to_far(p, p, k).wait_recv()
            small += far[p, (plane - k + planes) % planes]
        first_new, second_new, direction = moments(small, first[p], second[p])
        dirs[p, me] = direction
        squared = jnp.sum((direction * direction).reshape(rank_rows // 8, 8, width), axis=0)
        squares[p, tp] = sum(squared[:, low : low + 128] for low in range(0, width, 128))
        for k in range(1, tps):
            tell(p, k).start()
        first_out[p] = first_new
        second_out[p] = second_new

    def send(p):
        for k in order:
            spread(p, k).start()

    def add_squares(p):
        for k in range(1, tps):
            tell(p, k).wait_recv()
        sums[p, me] = jnp.sum(squares[p], axis=0)
        send(2 + p)

    def relay(p):
        for k in range(1, planes):
            spread(p, k).wait_recv()
            hand_on(p, k).start()

    def block(c, owner, low, size):
        return copies.at[c, pl.ds(pl.multiple_of(owner * rows + low, 16), size)]

    slabs = [(p, low) for p in range(2) for low in range(0, rows, E_ROWS)]

    def slab(owner, piece):
        p, low = slabs[piece]
        return block(p, owner, low, E_ROWS)

    outer = Ring(n, me, len(slabs), lambda piece: slab(me, piece), slab, ring_e_send, ring_e_recv)

    def renew(p):
        for q in (p, 2 + p):
            spread(q, 0).wait_recv()
            for k in range(1, planes):
                hand_on(q, k).wait_recv()
        square = jnp.sum(jnp.sum(sums[p], axis=0), keepdims=True)
        scale = 1.0 / jnp.maximum(jnp.sqrt(square / (rank * width * tps)), scale_floor)
        upper, lower = split_two(dirs[p].reshape(rank, width))
        made = jnp.dot(fac[p], upper, preferred_element_type=jnp.float32)
        made += jnp.dot(fac[p], lower, preferred_element_type=jnp.float32)
        step = -scale * made
        made = weight[p] + learn_rate * step
        block(p, me, 0, rows)[...] = made.astype(jnp.bfloat16)
        outer.begin([i for i in range(len(slabs)) if slabs[i][0] == p])
        update_out[p] = step
        new_out[p] = made

    move(0)
    send(0)
    move(1)
    add_squares(0)
    send(1)
    relay(0)
    relay(2)
    add_squares(1)
    renew(0)
    relay(1)
    relay(3)
    renew(1)
    for step in range(1, planes + 1):
        outer.step(step)
    ring.finish()
    for p, c in enumerate(chains):
        for k in order:
            to_near(p, c, k).wait_send()
            if k:
                to_far(p, c, k).wait_send()
    for p in range(4):
        for k in order:
            spread(p, k).wait_send()
            if k:
                hand_on(p, k).wait_send()
    for p in range(2):
        for k in range(1, tps):
            tell(p, k).wait_send()
    outer.finish()


def settle(count, *refs):
    sems = refs[3 * count]
    moves = []
    for i in range(count):
        for p in range(2):
            moves.append(pltpu.make_async_copy(refs[i].at[p], refs[(1 + p) * count + i], sems.at[p, i]))
    for move in moves:
        move.start()
    for move in moves:
        move.wait()


def fused_body(n, tps, *args):
    x, cot, _, fac, _, first, _, _, _, weight, _ = args
    bf16, f32 = jnp.bfloat16, jnp.float32
    rows, rank = fac.shape
    width = cot.shape[1]
    rank_rows = first.shape[0]
    planes = n // 2
    matrix = jax.ShapeDtypeStruct((rows, width), f32)
    copy = jax.ShapeDtypeStruct((rows * n, width), bf16)
    moment = jax.ShapeDtypeStruct((rank_rows, width), f32)
    outs = (matrix, matrix, copy, moment, moment)
    e_pieces = 2 * rows // E_ROWS
    dma = pltpu.SemaphoreType.DMA
    vmem = pltpu.VMEM
    made = pl.pallas_call(
        functools.partial(fused, n, tps),
        out_shape=tuple(jax.ShapeDtypeStruct((2,) + out.shape, out.dtype) for out in outs),
        in_specs=[pl.BlockSpec(memory_space=pltpu.HBM)] * 11,
        out_specs=(pl.BlockSpec(memory_space=pltpu.VMEM),) * 5,
        scratch_shapes=[
            vmem(x.shape, bf16),
            vmem((2,) + cot.shape, bf16),
            vmem((2,) + fac.shape, bf16),
            vmem((2,) + first.shape, f32),
            vmem((2,) + first.shape, f32),
            vmem((2, rows, width), f32),
            vmem((n,) + fac.shape, bf16),
            vmem((2, x.shape[0], rank), f32),
            vmem((2, n) + first.shape, f32),
            vmem((2, planes) + first.shape, f32),
            vmem((2, planes) + first.shape, f32),
            vmem((2, planes) + first.shape, f32),
            vmem((2, n) + first.shape, f32),
            vmem((2, tps, 8, 128), f32),
            vmem((2, n, 8, 128), f32),
            dma((11,)),
            dma((2, planes, A_PIECES)),
            dma((2, planes, A_PIECES)),
            dma((2, planes, e_pieces)),
            dma((2, planes, e_pieces)),
            dma,
            dma,
            dma((2, planes)),
            dma((2, planes)),
            dma((2, planes)),
            dma((2, planes)),
            dma((4, planes)),
            dma((4, planes)),
            dma((4, planes - 1)),
            dma((4, planes - 1)),
            dma((2, tps - 1)),
            dma((2, tps - 1)),
        ],
        compiler_params=pltpu.CompilerParams(
            collective_id=0, has_side_effects=True, vmem_limit_bytes=VMEM_GRANT
        ),
    )(*[pltpu.with_memory_space_constraint(arg, pltpu.HBM) for arg in args])
    done = pl.pallas_call(
        functools.partial(settle, len(outs)),
        out_shape=outs * 2,
        in_specs=[ANY] * len(outs),
        out_specs=(ANY,) * (2 * len(outs)),
        scratch_shapes=[dma((2, len(outs)))],
        compiler_params=pltpu.CompilerParams(vmem_limit_bytes=SMALL_GRANT),
    )(*made)
    return tuple(done)


def split_three(values):
    upper = lax.optimization_barrier(values.astype(jnp.bfloat16))
    rest = values - upper.astype(jnp.float32)
    middle = lax.optimization_barrier(rest.astype(jnp.bfloat16))
    lower = (rest - middle.astype(jnp.float32)).astype(jnp.bfloat16)
    return (upper, middle, lower)


def project_tokens(mixed, cotangent):
    contract = (((0,), (0,)), ((), ()))
    total = jnp.zeros((mixed.shape[1], cotangent.shape[1]), jnp.float32)
    for piece in split_three(mixed):
        total = total + lax.dot_general(
            piece, cotangent, contract, preferred_element_type=jnp.float32
        )
    return total


def plain_body(
    block_input,
    query_cotangent,
    key_cotangent,
    query_factor,
    key_factor,
    query_first,
    query_second,
    key_first,
    key_second,
    query_weight,
    key_weight,
):
    query_wide = query_factor.astype(jnp.float32)
    key_wide = key_factor.astype(jnp.float32)
    whole_query, whole_key = (
        lax.all_gather(query_factor, "fs", axis=0, tiled=True),
        lax.all_gather(key_factor, "fs", axis=0, tiled=True),
    )
    mixed_query = jnp.dot(block_input, whole_query, preferred_element_type=jnp.float32)
    mixed_key = jnp.dot(block_input, whole_key, preferred_element_type=jnp.float32)
    query_part = project_tokens(mixed_query, query_cotangent)
    key_part = project_tokens(mixed_key, key_cotangent)
    small_query, small_key = (
        lax.psum_scatter(query_part, "fs", scatter_dimension=0, tiled=True),
        lax.psum_scatter(key_part, "fs", scatter_dimension=0, tiled=True),
    )
    query_first_new, query_second_new, query_direction = moments(
        small_query, query_first, query_second
    )
    key_first_new, key_second_new, key_direction = moments(small_key, key_first, key_second)
    full_query, full_key = (
        lax.all_gather(query_direction, "fs", axis=0, tiled=True),
        lax.all_gather(key_direction, "fs", axis=0, tiled=True),
    )
    query_square, key_square = lax.psum(
        (jnp.sum(query_direction * query_direction), jnp.sum(key_direction * key_direction)),
        ("fs", "tp"),
    )
    entry_count = full_query.shape[0] * full_query.shape[1] * lax.axis_size("tp")
    query_scale = 1.0 / jnp.maximum(jnp.sqrt(query_square / entry_count), scale_floor)
    key_scale = 1.0 / jnp.maximum(jnp.sqrt(key_square / entry_count), scale_floor)
    query_update = -query_scale * jnp.dot(query_wide, full_query, precision=lax.Precision.HIGHEST)
    key_update = -key_scale * jnp.dot(key_wide, full_key, precision=lax.Precision.HIGHEST)
    query_new = query_weight + learn_rate * query_update
    key_new = key_weight + learn_rate * key_update
    query_copy, key_copy = (
        lax.all_gather(query_new.astype(jnp.bfloat16), "fs", axis=0, tiled=True),
        lax.all_gather(key_new.astype(jnp.bfloat16), "fs", axis=0, tiled=True),
    )
    return (
        query_update,
        query_new,
        query_copy,
        query_first_new,
        query_second_new,
        key_update,
        key_new,
        key_copy,
        key_first_new,
        key_second_new,
    )


def solution(mesh):
    n, tps = mesh.shape["fs"], mesh.shape["tp"]
    split = P("fs", "tp")
    in_specs = (P("fs", None), split, split, P("fs", None), P("fs", None)) + (split,) * 6
    out_specs = (split, split, P(None, "tp"), split, split) * 2

    def body(*args):
        factor, first = args[3], args[5]
        whole_tiles = first.shape[0] % 8 == 0 and factor.shape[0] % 128 == 0
        if n % 2 == 0 and tps % 2 == 0 and whole_tiles:
            return fused_body(n, tps, *args)
        return plain_body(*args)

    return jax.shard_map(body, mesh=mesh, in_specs=in_specs, out_specs=out_specs, check_vma=False)
```

```python
import functools

import jax
import jax.numpy as jnp
from jax import lax
from jax.experimental import pallas as pl
from jax.experimental.pallas import tpu as pltpu
from jax.sharding import PartitionSpec as P

beta_one = 0.9
beta_two = 0.99
denom_floor = 0.001
scale_floor = 0.5
learn_rate = 0.02
MESH = pl.DeviceIdType.MESH
VMEM_GRANT = 24 * 1024 * 1024
SMALL_GRANT = 1024 * 1024
A_PIECES = 4
E_ROWS = 64
ANY = pl.BlockSpec(memory_space=pl.ANY)


def moments(small, first, second):
    first_new = beta_one * first + (1.0 - beta_one) * small
    second_new = beta_two * second + (1.0 - beta_two) * small * small
    direction = first_new / (jnp.sqrt(second_new) + denom_floor)
    return (first_new, second_new, direction)


def split_two(values):
    upper = values.astype(jnp.bfloat16)
    lower = (values - upper.astype(jnp.float32)).astype(jnp.bfloat16)
    return (upper, lower)


def ring_place(index, n):
    odd = index % 2
    along = index // 2
    return (1 - odd) * along + odd * (n - 1 - along)


def ring_index(place, n):
    back = place // (n // 2)
    return (1 - back) * (2 * place) + back * (2 * (n - 1 - place) + 1)


class Ring:
    def __init__(self, n, me, pieces, own, slot, send, recv):
        self.n, self.me, self.pieces = n, me, pieces
        self.own, self.slot, self.send, self.recv = own, slot, send, recv
        self.place = ring_place(me, n)
        self.last = n // 2

    def active(self, step, way, piece):
        return step < self.last or (step == self.last and way == piece % 2)

    def owner(self, step, way):
        shift = -step if way == 0 else step
        return ring_index((self.place + shift + self.n) % self.n, self.n)

    def copy(self, step, way, piece):
        shift = 1 if way == 0 else self.n - 1
        to = ring_index((self.place + shift) % self.n, self.n)
        if step == 1:
            owner, src = self.me, self.own(piece)
        else:
            owner = self.owner(step - 1, way)
            src = self.slot(owner, piece)
        return pltpu.make_async_remote_copy(
            src_ref=src,
            dst_ref=self.slot(owner, piece),
            send_sem=self.send.at[way, step - 1, piece],
            recv_sem=self.recv.at[way, step - 1, piece],
            device_id={"fs": to},
            device_id_type=MESH,
        )

    def begin(self, pieces):
        for piece in pieces:
            for way in range(2):
                if self.active(1, way, piece):
                    self.copy(1, way, piece).start()

    def step(self, step):
        for piece in range(self.pieces):
            for way in range(2):
                if self.active(step, way, piece):
                    self.copy(step, way, piece).wait_recv()
                    if self.active(step + 1, way, piece):
                        self.copy(step + 1, way, piece).start()

    def finish(self):
        for step in range(1, self.last + 1):
            for way in range(2):
                for piece in range(self.pieces):
                    if self.active(step, way, piece):
                        self.copy(step, way, piece).wait_send()


def fused(
    n,
    tps,
    x_in,
    cq_in,
    ck_in,
    fq_in,
    fk_in,
    q1_in,
    q2_in,
    k1_in,
    k2_in,
    wq_in,
    wk_in,
    update_out,
    new_out,
    copies,
    first_out,
    second_out,
    x,
    cot,
    fac,
    first,
    second,
    weight,
    gathered,
    mix,
    part,
    near,
    paired,
    far,
    dirs,
    squares,
    sums,
    in_sem,
    ring_a_send,
    ring_a_recv,
    ring_e_send,
    ring_e_recv,
    mix_send,
    mix_recv,
    near_send,
    near_recv,
    far_send,
    far_recv,
    dir_send,
    dir_recv,
    pass_send,
    pass_recv,
    sq_send,
    sq_recv,
):
    me = lax.axis_index("fs")
    tp = lax.axis_index("tp")
    core = tp % 2
    chains = (0, 1)
    rows = fac.shape[1]
    rank_rows = first.shape[1]
    rank = n * rank_rows
    width = cot.shape[2]
    planes = n // 2
    side = me % 2
    plane = me // 2
    twin = me + 1 - 2 * side

    loads = [
        pltpu.make_async_copy(src, dst, in_sem.at[i])
        for i, (src, dst) in enumerate(
            (
                (fq_in, fac.at[0]),
                (fk_in, fac.at[1]),
                (x_in, x),
                (cq_in, cot.at[0]),
                (ck_in, cot.at[1]),
                (wq_in, weight.at[0]),
                (wk_in, weight.at[1]),
                (q1_in, first.at[0]),
                (k1_in, first.at[1]),
                (q2_in, second.at[0]),
                (k2_in, second.at[1]),
            )
        )
    ]
    for load in loads:
        load.start()

    barrier = pltpu.get_barrier_semaphore()
    place = ring_place(me, n)
    for shift in (1, n - 1):
        to = ring_index((place + shift) % n, n)
        pl.semaphore_signal(barrier, inc=1, device_id={"fs": to}, device_id_type=MESH)
    for k in range(1, tps):
        pl.semaphore_signal(barrier, inc=1, device_id={"tp": (tp + k) % tps}, device_id_type=MESH)
    pl.semaphore_wait(barrier, 2 + tps - 1)

    loads[0].wait()
    loads[1].wait()
    cut = rows // A_PIECES
    ring = Ring(
        n,
        me,
        A_PIECES,
        lambda piece: fac.at[core, pl.ds(piece * cut, cut)],
        lambda owner, piece: gathered.at[owner, pl.ds(piece * cut, cut)],
        ring_a_send,
        ring_a_recv,
    )
    ring.begin(range(A_PIECES))
    loads[2].wait()

    def product(owner, block):
        columns = pl.ds(pl.multiple_of(owner * rows, 128), rows)
        return jnp.dot(x[:, columns], block, preferred_element_type=jnp.float32)

    mixed = product(me, fac[core])
    for step in range(1, planes):
        ring.step(step)
        for way in range(2):
            owner = ring.owner(step, way)
            mixed += product(owner, gathered[owner])
    loads[5].wait()
    loads[6].wait()
    ring.step(planes)
    owner = ring.owner(planes, 0)
    mix[core] = mixed + product(owner, gathered[owner])

    swap = pltpu.make_async_remote_copy(
        src_ref=mix.at[core],
        dst_ref=mix.at[core],
        send_sem=mix_send,
        recv_sem=mix_recv,
        device_id={"tp": tp + 1 - 2 * core},
        device_id_type=MESH,
    )
    swap.start()
    loads[3].wait()
    loads[4].wait()

    def to_near(p, c, k):
        to = (plane + k) % planes
        return pltpu.make_async_remote_copy(
            src_ref=part.at[c, 2 * to + 1 - side],
            dst_ref=near.at[c, to],
            send_sem=near_send.at[p, k],
            recv_sem=near_recv.at[p, k],
            device_id={"fs": twin},
            device_id_type=MESH,
        )

    def to_far(p, c, k):
        to = (plane + k) % planes
        return pltpu.make_async_remote_copy(
            src_ref=paired.at[c, to],
            dst_ref=far.at[c, plane],
            send_sem=far_send.at[p, k],
            recv_sem=far_recv.at[p, k],
            device_id={"fs": 2 * to + side},
            device_id_type=MESH,
        )

    order = tuple(range(1, planes)) + (0,)
    contract = (((0,), (0,)), ((), ()))
    for p, c in enumerate(chains):
        if p == 0:
            swap.wait()
        upper, lower = split_two(mix[c])
        total = lax.dot_general(upper, cot[c], contract, preferred_element_type=jnp.float32)
        total += lax.dot_general(lower, cot[c], contract, preferred_element_type=jnp.float32)
        part[c] = total.reshape(n, rank_rows, width)
        for k in order:
            to_near(p, c, k).start()
    for load in loads[7:]:
        load.wait()
    for p, c in enumerate(chains):
        for k in order:
            to_near(p, c, k).wait_recv()
            to = (plane + k) % planes
            paired[c, to] = part[c, 2 * to + side] + near[c, to]
            if k:
                to_far(p, c, k).start()

    def held(p, owner):
        return sums.at[p - 2, owner] if p >= 2 else dirs.at[p, owner]

    def spread(p, k):
        to = 2 * ((plane + k) % planes) + side if k else twin
        return pltpu.make_async_remote_copy(
            src_ref=held(p, me),
            dst_ref=held(p, me),
            send_sem=dir_send.at[p, k],
            recv_sem=dir_recv.at[p, k],
            device_id={"fs": to},
            device_id_type=MESH,
        )

    def hand_on(p, k):
        owner = 2 * ((plane - k + planes) % planes) + side
        return pltpu.make_async_remote_copy(
            src_ref=held(p, owner),
            dst_ref=held(p, owner),
            send_sem=pass_send.at[p, k - 1],
            recv_sem=pass_recv.at[p, k - 1],
            device_id={"fs": twin},
            device_id_type=MESH,
        )

    def tell(p, k):
        return pltpu.make_async_remote_copy(
            src_ref=squares.at[p, tp],
            dst_ref=squares.at[p, tp],
            send_sem=sq_send.at[p, k - 1],
            recv_sem=sq_recv.at[p, k - 1],
            device_id={"tp": (tp + k) % tps},
            device_id_type=MESH,
        )

    def move(p):
        small = paired[p, plane]
        for k in range(1, planes):
            to_far(p, p, k).wait_recv()
            small += far[p, (plane - k + planes) % planes]
        first_new, second_new, direction = moments(small, first[p], second[p])
        dirs[p, me] = direction
        squared = jnp.sum((direction * direction).reshape(rank_rows // 8, 8, width), axis=0)
        squares[p, tp] = sum(squared[:, low : low + 128] for low in range(0, width, 128))
        for k in range(1, tps):
            tell(p, k).start()
        first_out[p] = first_new
        second_out[p] = second_new

    def send(p):
        for k in order:
            spread(p, k).start()

    def add_squares(p):
        for k in range(1, tps):
            tell(p, k).wait_recv()
        sums[p, me] = jnp.sum(squares[p], axis=0)
        send(2 + p)

    def relay(p):
        for k in range(1, planes):
            spread(p, k).wait_recv()
            hand_on(p, k).start()

    def block(c, owner, low, size):
        return copies.at[c, pl.ds(pl.multiple_of(owner * rows + low, 16), size)]

    slabs = [(p, low) for p in range(2) for low in range(0, rows, E_ROWS)]

    def slab(owner, piece):
        p, low = slabs[piece]
        return block(p, owner, low, E_ROWS)

    outer = Ring(n, me, len(slabs), lambda piece: slab(me, piece), slab, ring_e_send, ring_e_recv)

    def renew(p):
        for q in (p, 2 + p):
            spread(q, 0).wait_recv()
            for k in range(1, planes):
                hand_on(q, k).wait_recv()
        square = jnp.sum(jnp.sum(sums[p], axis=0), keepdims=True)
        scale = 1.0 / jnp.maximum(jnp.sqrt(square / (rank * width * tps)), scale_floor)
        upper, lower = split_two(dirs[p].reshape(rank, width))
        made = jnp.dot(fac[p], upper, preferred_element_type=jnp.float32)
        made += jnp.dot(fac[p], lower, preferred_element_type=jnp.float32)
        step = -scale * made
        made = weight[p] + learn_rate * step
        block(p, me, 0, rows)[...] = made.astype(jnp.bfloat16)
        outer.begin([i for i in range(len(slabs)) if slabs[i][0] == p])
        update_out[p] = step
        new_out[p] = made

    move(0)
    send(0)
    move(1)
    add_squares(0)
    send(1)
    relay(0)
    relay(2)
    add_squares(1)
    relay(1)
    renew(0)
    relay(3)
    renew(1)
    for step in range(1, planes + 1):
        outer.step(step)
    ring.finish()
    for p, c in enumerate(chains):
        for k in order:
            to_near(p, c, k).wait_send()
            if k:
                to_far(p, c, k).wait_send()
    for p in range(4):
        for k in order:
            spread(p, k).wait_send()
            if k:
                hand_on(p, k).wait_send()
    for p in range(2):
        for k in range(1, tps):
            tell(p, k).wait_send()
    outer.finish()


def settle(count, *refs):
    sems = refs[3 * count]
    moves = []
    for i in range(count):
        for p in range(2):
            moves.append(pltpu.make_async_copy(refs[i].at[p], refs[(1 + p) * count + i], sems.at[p, i]))
    for move in moves:
        move.start()
    for move in moves:
        move.wait()


def fused_body(n, tps, *args):
    x, cot, _, fac, _, first, _, _, _, weight, _ = args
    bf16, f32 = jnp.bfloat16, jnp.float32
    rows, rank = fac.shape
    width = cot.shape[1]
    rank_rows = first.shape[0]
    planes = n // 2
    matrix = jax.ShapeDtypeStruct((rows, width), f32)
    copy = jax.ShapeDtypeStruct((rows * n, width), bf16)
    moment = jax.ShapeDtypeStruct((rank_rows, width), f32)
    outs = (matrix, matrix, copy, moment, moment)
    e_pieces = 2 * rows // E_ROWS
    dma = pltpu.SemaphoreType.DMA
    vmem = pltpu.VMEM
    made = pl.pallas_call(
        functools.partial(fused, n, tps),
        out_shape=tuple(jax.ShapeDtypeStruct((2,) + out.shape, out.dtype) for out in outs),
        in_specs=[pl.BlockSpec(memory_space=pltpu.HBM)] * 11,
        out_specs=(pl.BlockSpec(memory_space=pltpu.VMEM),) * 5,
        scratch_shapes=[
            vmem(x.shape, bf16),
            vmem((2,) + cot.shape, bf16),
            vmem((2,) + fac.shape, bf16),
            vmem((2,) + first.shape, f32),
            vmem((2,) + first.shape, f32),
            vmem((2, rows, width), f32),
            vmem((n,) + fac.shape, bf16),
            vmem((2, x.shape[0], rank), f32),
            vmem((2, n) + first.shape, f32),
            vmem((2, planes) + first.shape, f32),
            vmem((2, planes) + first.shape, f32),
            vmem((2, planes) + first.shape, f32),
            vmem((2, n) + first.shape, f32),
            vmem((2, tps, 8, 128), f32),
            vmem((2, n, 8, 128), f32),
            dma((11,)),
            dma((2, planes, A_PIECES)),
            dma((2, planes, A_PIECES)),
            dma((2, planes, e_pieces)),
            dma((2, planes, e_pieces)),
            dma,
            dma,
            dma((2, planes)),
            dma((2, planes)),
            dma((2, planes)),
            dma((2, planes)),
            dma((4, planes)),
            dma((4, planes)),
            dma((4, planes - 1)),
            dma((4, planes - 1)),
            dma((2, tps - 1)),
            dma((2, tps - 1)),
        ],
        compiler_params=pltpu.CompilerParams(
            collective_id=0, has_side_effects=True, vmem_limit_bytes=VMEM_GRANT
        ),
    )(*[pltpu.with_memory_space_constraint(arg, pltpu.HBM) for arg in args])
    done = pl.pallas_call(
        functools.partial(settle, len(outs)),
        out_shape=outs * 2,
        in_specs=[ANY] * len(outs),
        out_specs=(ANY,) * (2 * len(outs)),
        scratch_shapes=[dma((2, len(outs)))],
        compiler_params=pltpu.CompilerParams(vmem_limit_bytes=SMALL_GRANT),
    )(*made)
    return tuple(done)


def split_three(values):
    upper = lax.optimization_barrier(values.astype(jnp.bfloat16))
    rest = values - upper.astype(jnp.float32)
    middle = lax.optimization_barrier(rest.astype(jnp.bfloat16))
    lower = (rest - middle.astype(jnp.float32)).astype(jnp.bfloat16)
    return (upper, middle, lower)


def project_tokens(mixed, cotangent):
    contract = (((0,), (0,)), ((), ()))
    total = jnp.zeros((mixed.shape[1], cotangent.shape[1]), jnp.float32)
    for piece in split_three(mixed):
        total = total + lax.dot_general(
            piece, cotangent, contract, preferred_element_type=jnp.float32
        )
    return total


def plain_body(
    block_input,
    query_cotangent,
    key_cotangent,
    query_factor,
    key_factor,
    query_first,
    query_second,
    key_first,
    key_second,
    query_weight,
    key_weight,
):
    query_wide = query_factor.astype(jnp.float32)
    key_wide = key_factor.astype(jnp.float32)
    whole_query, whole_key = (
        lax.all_gather(query_factor, "fs", axis=0, tiled=True),
        lax.all_gather(key_factor, "fs", axis=0, tiled=True),
    )
    mixed_query = jnp.dot(block_input, whole_query, preferred_element_type=jnp.float32)
    mixed_key = jnp.dot(block_input, whole_key, preferred_element_type=jnp.float32)
    query_part = project_tokens(mixed_query, query_cotangent)
    key_part = project_tokens(mixed_key, key_cotangent)
    small_query, small_key = (
        lax.psum_scatter(query_part, "fs", scatter_dimension=0, tiled=True),
        lax.psum_scatter(key_part, "fs", scatter_dimension=0, tiled=True),
    )
    query_first_new, query_second_new, query_direction = moments(
        small_query, query_first, query_second
    )
    key_first_new, key_second_new, key_direction = moments(small_key, key_first, key_second)
    full_query, full_key = (
        lax.all_gather(query_direction, "fs", axis=0, tiled=True),
        lax.all_gather(key_direction, "fs", axis=0, tiled=True),
    )
    query_square, key_square = lax.psum(
        (jnp.sum(query_direction * query_direction), jnp.sum(key_direction * key_direction)),
        ("fs", "tp"),
    )
    entry_count = full_query.shape[0] * full_query.shape[1] * lax.axis_size("tp")
    query_scale = 1.0 / jnp.maximum(jnp.sqrt(query_square / entry_count), scale_floor)
    key_scale = 1.0 / jnp.maximum(jnp.sqrt(key_square / entry_count), scale_floor)
    query_update = -query_scale * jnp.dot(query_wide, full_query, precision=lax.Precision.HIGHEST)
    key_update = -key_scale * jnp.dot(key_wide, full_key, precision=lax.Precision.HIGHEST)
    query_new = query_weight + learn_rate * query_update
    key_new = key_weight + learn_rate * key_update
    query_copy, key_copy = (
        lax.all_gather(query_new.astype(jnp.bfloat16), "fs", axis=0, tiled=True),
        lax.all_gather(key_new.astype(jnp.bfloat16), "fs", axis=0, tiled=True),
    )
    return (
        query_update,
        query_new,
        query_copy,
        query_first_new,
        query_second_new,
        key_update,
        key_new,
        key_copy,
        key_first_new,
        key_second_new,
    )


def solution(mesh):
    n, tps = mesh.shape["fs"], mesh.shape["tp"]
    split = P("fs", "tp")
    in_specs = (P("fs", None), split, split, P("fs", None), P("fs", None)) + (split,) * 6
    out_specs = (split, split, P(None, "tp"), split, split) * 2

    def body(*args):
        factor, first = args[3], args[5]
        whole_tiles = first.shape[0] % 8 == 0 and factor.shape[0] % 128 == 0
        if n % 2 == 0 and tps % 2 == 0 and whole_tiles:
            return fused_body(n, tps, *args)
        return plain_body(*args)

    return jax.shard_map(body, mesh=mesh, in_specs=in_specs, out_specs=out_specs, check_vma=False)
```
